32 devices in a mesh: fs: 4 (over y, x), tp: 8 (over z, core).
Axes of the slice: x: 2, y: 2, z: 4, core: 2. Of those that a mesh axis runs over, the one named last changes fastest.
Arguments:
- prompt: bfloat16 [4096, 2048], P(('fs', 'tp')), may hold values from -6 to 6
- norm_gain: float32 [2048], P('tp'), may hold values from 0.1 to 1.9
- gate_master: float32 [8, 2, 512, 2048], P(None, None, 'fs', 'tp'), may hold values from -0.125 to 0.125
- up_master: float32 [8, 2, 512, 2048], P(None, None, 'fs', 'tp'), may hold values from -0.125 to 0.125
- down_master: float32 [8, 2, 512, 2048], P(None, None, 'fs', 'tp'), may hold values from -0.25 to 0.25
- group_pick: int32 [4096, 1], P(('fs', 'tp')), may hold values from 0 to 7; in each aligned block of 128 rows (0 to 127, 128 to 255, ...) at most 32 rows name the same one
- route_weight: bfloat16 [4096, 2], P(('fs', 'tp')), may hold values from 0.099609375 to 1
Outputs:
- gate_serve: bfloat16 [8, 2, 512, 2048], P('tp', None, 'fs')
- up_serve: bfloat16 [8, 2, 512, 2048], P('tp', None, 'fs')
- down_serve: bfloat16 [8, 2, 512, 2048], P('tp', None, 'fs')
- mixed: bfloat16 [4096, 2048], P(('fs', 'tp'))
The draws below stay inside these ranges and needn't reach their ends.
Inputs may be any that keep to these rules, and one draw needn't show every extreme that they name: `group_pick`: in the rows of one device no group is named by more than 32 rows, and in every draw some device's rows name one group exactly 32 times.
All inputs are finite; a program needn't handle non-finite values.
Results may differ from the reference program's by a relative error of at most 0.0081.
Values may be sent and summed in bfloat16 or wider, within the bound.
A program may use at most 64 MiB of HBM per device.

```python
import math
import jax
import jax.numpy as jnp
import numpy as np
from jax import lax

D = 2048
HID = 512
EXP_GRP = 2
TOK_DEV = 128
GROUPS = 8
CAP = 32
TOKENS = 4096


def steps_of(key, shape, shards, smallest, high):
    gain = 1.0
    for position, shards_of in shards:
        heights = jax.random.uniform(jax.random.fold_in(jax.random.fold_in(key, 6), position), (shards_of,), jnp.float32, smallest / len(shards), high / len(shards))
        gain = gain * jnp.repeat(jnp.exp(heights), shape[position] // shards_of).reshape((-1,) + (1,) * (len(shape) - 1 - position))
    return gain


def assign_block(rng, own, number, rows, number_of, top, bound, skew):
    ranking = jax.random.permutation(rng, number_of)
    packed, ordinary = load_shares(number_of, rows * top, bound, skew, True), load_shares(number_of, rows * top, bound, skew, False)
    places = jnp.arange(number_of)

    def named(sizes, rotation):
        used = int((sizes > 0).sum())
        fixed = max(1, used // 4)
        passed = fixed + (places - fixed + rotation * (used - fixed)) % max(1, number_of - fixed)
        return jnp.zeros((number_of,), jnp.int32).at[ranking[jnp.where(places < fixed, places, passed)]].set(jnp.asarray(sizes, jnp.int32))

    sizes = jnp.where(number % 4 == 0, named(packed, number // 4), named(ordinary, number - number // 4 - 1))
    mixed = jax.random.permutation(jax.random.fold_in(own, 3), number_of)
    source_of, taker = mixed[0:number_of // 2 * 2:2], mixed[1:number_of // 2 * 2:2]
    slack = jnp.minimum(sizes[source_of] - 1, bound - sizes[taker]) // 2
    slack = jnp.where((source_of == ranking[0]) | (taker == ranking[0]) | (sizes[taker] == 0), 0, jnp.maximum(slack, 0))
    passed = jax.random.randint(jax.random.fold_in(own, 4), (number_of // 2,), 0, 1 << 20) % (slack + 1)
    sizes = sizes.at[source_of].add(-passed).at[taker].add(passed)
    items = jnp.searchsorted(jnp.cumsum(sizes), jnp.arange(rows * top), side="right").astype(jnp.int32)
    grid = items.reshape(top, rows).T
    grid = grid[jax.random.permutation(jax.random.fold_in(own, 1), rows)]
    rotation = jax.random.randint(jax.random.fold_in(own, 2), (rows, 1), 0, top)
    return jnp.take_along_axis(grid, (jnp.arange(top)[None, :] + rotation) % top, axis=1)


def load_shares(amount, total, reach, skew, full):
    loads = [(1 << 20) // math.isqrt(standing ** skew) + 1 for standing in range(1, amount + 1)]
    largest = reach if full else min(reach, max(-(-total // amount), total * loads[0] // sum(loads)))
    least = 1 if total - largest >= amount - 1 else 0
    given, surplus = [largest] + [least] * (amount - 1), total - largest - least * (amount - 1)
    while surplus > 0:
        movable = [i for i in range(1, amount) if given[i] < largest] or [i for i in range(1, amount) if given[i] < reach]
        whole, budget = sum([loads[i] for i in movable]), surplus
        for i in movable:
            addition = min(reach - given[i], max(1, budget * loads[i] // whole), surplus)
            given[i] = given[i] + addition
            surplus = surplus - addition
    return np.array(given)


def normal_values(own_key, dims, spread, limit, pieces=(), kind=jnp.bfloat16):
    entries = spread * jax.random.normal(own_key, dims, jnp.float32)
    if pieces:
        entries = entries * steps_of(own_key, dims, pieces, -0.22, 0.18)
    return jnp.clip(entries, -limit, limit).astype(kind)


def setup_inputs(seed: int = 0) -> dict:
    splits = jax.random.split(jax.random.key(seed), 8)
    prompt = normal_values(splits[0], (TOKENS, D), 1.0, 6.0, ((0, 32),))
    norm_gain = jnp.clip(1.0 + 0.18 * jax.random.normal(splits[1], (D,), jnp.float32), 0.1, 1.9)
    gate_master = normal_values(splits[2], (GROUPS, EXP_GRP, HID, D), D ** -0.5, 0.125, ((2, 4), (3, 8)), jnp.float32)
    up_master = normal_values(splits[3], (GROUPS, EXP_GRP, HID, D), D ** -0.5, 0.125, ((2, 4), (3, 8)), jnp.float32)
    down_master = normal_values(splits[4], (GROUPS, EXP_GRP, HID, D), HID ** -0.5, 0.25, ((2, 4), (3, 8)), jnp.float32)
    group_pick_keys = jax.random.split(jax.random.fold_in(splits[5], 1), TOKENS // TOK_DEV)
    group_pick_turns = jax.random.permutation(jax.random.fold_in(splits[5], 3), TOKENS // TOK_DEV)
    group_pick = jax.vmap(lambda own, number: assign_block(jax.random.fold_in(splits[5], 2), own, number, TOK_DEV, GROUPS, 1, CAP, 2))(group_pick_keys, group_pick_turns).reshape((TOKENS, 1))
    route_weight = jnp.clip(jnp.exp(math.log(1.0) - 2.306499 * jax.random.uniform(splits[6], (TOKENS, EXP_GRP), jnp.float32) ** steps_of(splits[6], (TOKENS, EXP_GRP), ((0, 32),), -0.2, 0.2)), 0.099609375, 1.0).astype(jnp.bfloat16)
    return dict(prompt=prompt, norm_gain=norm_gain, gate_master=gate_master, up_master=up_master, down_master=down_master, group_pick=group_pick, route_weight=route_weight)


EPS = 1e-06

def reference(prompt, norm_gain, gate_master, up_master, down_master, group_pick, route_weight):
    gate_serve = (gate_master * norm_gain).astype(jnp.bfloat16)
    up_serve = (up_master * norm_gain).astype(jnp.bfloat16)
    down_serve = down_master.astype(jnp.bfloat16)
    values = prompt.astype(jnp.float32)
    normed = (values * lax.rsqrt(lax.optimization_barrier(jnp.mean(values * values, axis=1, keepdims=True)) + EPS)).astype(jnp.bfloat16)
    chosen = group_pick[:, 0].astype(jnp.int32)
    order = jnp.argsort(chosen, stable=True).astype(jnp.int32)
    member = (chosen[:, None] == jnp.arange(GROUPS, dtype=jnp.int32)[None, :]).astype(jnp.int32)
    counts = lax.optimization_barrier(jnp.sum(member, axis=0)).astype(jnp.int32)
    starts = (jnp.cumsum(counts) - counts).astype(jnp.int32)
    row_bound = CAP * (TOKENS // TOK_DEV)
    slot_ids = jnp.arange(row_bound, dtype=jnp.int32)

    def one_group(running, group_index):
        slot_place = jnp.minimum(starts[group_index] + slot_ids, TOKENS - 1).astype(jnp.int32)
        token_ids = order[slot_place].astype(jnp.int32)
        is_valid = slot_ids < counts[group_index]
        group_rows = normed[token_ids].astype(jnp.float32)
        weights = jnp.where(is_valid[:, None], route_weight[token_ids].astype(jnp.float32), 0.0)
        gate_pre = jnp.einsum('sd,ehd->seh', group_rows, gate_serve[group_index].astype(jnp.float32))
        up_pre = jnp.einsum('sd,ehd->seh', group_rows, up_serve[group_index].astype(jnp.float32))
        hidden = (weights[:, :, None] * (jax.nn.silu(gate_pre) * up_pre)).astype(jnp.bfloat16)
        expert_out = jnp.einsum('seh,ehd->sd', hidden.astype(jnp.float32), down_serve[group_index].astype(jnp.float32)).astype(jnp.bfloat16)
        expert_out = jnp.where(is_valid[:, None], expert_out, jnp.zeros_like(expert_out))
        running = running.at[token_ids].add(expert_out)
        return (running, None)
    mixed, _ = lax.scan(one_group, jnp.zeros((TOKENS, D), jnp.bfloat16), jnp.arange(GROUPS, dtype=jnp.int32))
    return (gate_serve, up_serve, down_serve, mixed)
```

```python
import functools

import jax
import jax.numpy as jnp
from jax import lax
from jax.experimental import pallas as pl
from jax.experimental.pallas import tpu as pltpu
from jax.sharding import PartitionSpec as P

EPS = 1e-06
MESH = pl.DeviceIdType.MESH
LANES = 128
NT = (((1,), (1,)), ((), ()))
TN = (((0,), (0,)), ((), ()))


def expert_rows(group_rows, weights, pieces):
    gate_piece, up_piece, down_piece = pieces
    expert_count = gate_piece.shape[1]
    unit_count = gate_piece.shape[2]
    model_width = gate_piece.shape[3]
    row_count = group_rows.shape[0]
    gate_matrix = gate_piece.reshape(expert_count * unit_count, model_width)
    up_matrix = up_piece.reshape(expert_count * unit_count, model_width)
    down_matrix = down_piece.reshape(expert_count * unit_count, model_width)
    gate_pre = jnp.einsum("sd,hd->sh", group_rows, gate_matrix, preferred_element_type=jnp.float32)
    up_pre = jnp.einsum("sd,hd->sh", group_rows, up_matrix, preferred_element_type=jnp.float32)
    active = (jax.nn.silu(gate_pre) * up_pre).reshape(row_count, expert_count, unit_count)
    hidden = (weights.astype(jnp.float32)[:, :, None] * active).reshape(
        row_count, expert_count * unit_count
    )
    hidden = hidden.astype(jnp.bfloat16)
    return jnp.dot(hidden, down_matrix, preferred_element_type=jnp.float32)


def flipped(index, mask, size):
    total, bit = 0, 1
    while bit < size:
        digit = lax.rem(lax.div(index, bit), 2)
        total = total + bit * ((1 - digit) if mask & bit else digit)
        bit *= 2
    return total


def exchange_kernel(
    dims,
    prompt_in, gain_in, gate_in, up_in, down_in, pick_in, route_in,
    gate_out, up_out, down_out, ret, placing_ref,
    gain_ref, pick_ref, route_ref, down_all, prompt, stage, wsend, rows, xrows, acc, hid, hcat, rsum, route_pad,
    load, rows_s, rows_r, w_s, w_r, fx_s, fx_r, dx_s, dx_r, h_s, h_r, ret_s, ret_r, loc,
):
    fs_n, tp_n, experts, units, width, model, cap = dims
    flat, block, tokens = experts * units, tp_n * cap, prompt.shape[0]
    f = lax.axis_index("fs")
    t = lax.axis_index("tp")
    tp_peer = [flipped(t, k, tp_n) for k in range(tp_n)]
    fs_peer = [flipped(f, j, fs_n) for j in range(fs_n)]

    near = list(range(2, tp_n)) + [1]
    late = [tp_n // 2, tp_n // 2 + 1]
    early = [k for k in near if k not in late]
    pairs = list(range(0, tp_n, 2))
    down_order = early + late

    prompt_load = pltpu.make_async_copy(prompt_in, prompt, load.at[3, 0])
    small_loads = [
        pltpu.make_async_copy(src, dst, load.at[3, 1 + i])
        for i, (src, dst) in enumerate(
            ((pick_in, pick_ref), (route_in, route_ref), (gain_in, gain_ref))
        )
    ]
    for copy in small_loads:
        copy.start()
    prompt_load.start()
    sources = (gate_in, up_in, down_in)
    loads = {}

    def load_weight(m, k):
        loads[m, k] = pltpu.make_async_copy(
            sources[m].at[tp_peer[k]], stage.at[m, k], load.at[m, k]
        )
        loads[m, k].start()

    for k in early:
        load_weight(2, k)
    for m in range(2):
        for k in near:
            load_weight(m, k)
    for k in late:
        load_weight(2, k)
    for m in range(3):
        load_weight(m, 0)

    barrier = pltpu.get_barrier_semaphore()
    for k in range(1, tp_n):
        pl.semaphore_signal(barrier, inc=1, device_id=(f, tp_peer[k]), device_id_type=MESH)
    for j in range(1, fs_n):
        pl.semaphore_signal(barrier, inc=1, device_id=(fs_peer[j], t), device_id_type=MESH)

    def columns(index):
        return pl.ds(pl.multiple_of(index * width, width), width)

    def remote(src, dst, send, recv, fs_to, tp_to):
        return pltpu.make_async_remote_copy(
            src_ref=src, dst_ref=dst, send_sem=send, recv_sem=recv,
            device_id=(fs_to, tp_to), device_id_type=MESH,
        )

    for copy in small_loads:
        copy.wait()
    pick = pick_ref[...].astype(jnp.float32)
    group_id = lax.broadcasted_iota(jnp.int32, (tp_n, tokens), 0).astype(jnp.float32)
    member = jnp.where(group_id == pick, 1.0, 0.0)
    ahead = jnp.where(
        lax.broadcasted_iota(jnp.int32, (tokens, tokens), 0)
        <= lax.broadcasted_iota(jnp.int32, (tokens, tokens), 1),
        1.0, 0.0,
    ).astype(jnp.bfloat16)
    count = jnp.dot(member.astype(jnp.bfloat16), ahead, preferred_element_type=jnp.float32)
    rank = jnp.sum(member * count, axis=0, keepdims=True) - 1.0
    target = pick * cap + rank
    slot = lax.broadcasted_iota(jnp.int32, (block, tokens), 0).astype(jnp.float32)
    placing = jnp.where(slot == target, 1.0, 0.0).astype(jnp.bfloat16)
    placing_ref[...] = placing
    route_pad[...] = jnp.zeros_like(route_pad)
    route_pad[0:experts, :] = route_ref[...]
    routed = lax.dot_general(placing, route_pad[...], NT, preferred_element_type=jnp.float32)
    rows[:, :, model:] = routed.astype(jnp.bfloat16).reshape(tp_n, cap, LANES)
    prompt_load.wait()
    values = prompt[...].astype(jnp.float32)
    scale = lax.rsqrt(jnp.mean(values * values, axis=1, keepdims=True) + EPS)
    normed = (values * scale).astype(jnp.bfloat16)
    rows[:, :, :model] = (
        jnp.dot(placing, normed, preferred_element_type=jnp.float32)
        .astype(jnp.bfloat16)
        .reshape(tp_n, cap, model)
    )

    pl.semaphore_wait(barrier, tp_n - 1 + fs_n - 1)

    rows_copy = {}
    for k in near:
        rows_copy[k] = remote(
            rows.at[tp_peer[k]], xrows.at[f, t], rows_s.at[k], rows_r.at[k], f, tp_peer[k]
        )
        rows_copy[k].start()
    own_rows = pltpu.make_async_copy(rows.at[t], xrows.at[f, t], loc.at[0])
    own_rows.start()

    own_down = pl.ds(pl.multiple_of(f * flat, flat), flat)

    def landing(m):
        if m == 2:
            return down_all.at[own_down, columns(t)]
        return (gate_out, up_out)[m].at[:, columns(t)]

    w_copy = {}

    def convert(m, k):
        loads[m, k].wait()
        value = stage[m, k]
        if m < 2:
            value = value * gain_ref[...]
        value = value.astype(jnp.bfloat16)
        if k > 0:
            wsend[m, k] = value
            w_copy[m, k] = remote(
                wsend.at[m, k], landing(m), w_s.at[m, k], w_r.at[m, k], f, tp_peer[k]
            )
        elif m == 2:
            down_all[own_down, columns(t)] = value
        else:
            (gate_out, up_out)[m][:, columns(t)] = value

    for k in early:
        convert(2, k)
    for k in early:
        w_copy[2, k].start()
    for k in near:
        convert(0, k)
    for k in late:
        w_copy[0, k].start()
    for m in range(3):
        convert(m, 0)

    def spread(copies, k, piece, send, recv):
        first, second = (1, 2) if (k // 2 + k) % 2 == 0 else (2, 1)
        origin = {0: f, 1: fs_peer[first], 2: fs_peer[second]}

        def go(slot, owner, to):
            ref = piece(owner)
            copies[k, slot] = remote(
                ref, ref, send.at[k, slot], recv.at[k, slot], fs_peer[to], t
            )
            copies[k, slot].start()

        def own():
            go(0, f, first)
            go(1, f, second)

        def relay():
            copies[k, 0].wait_recv()
            go(2, fs_peer[first], second)

        return own, relay

    fx, dx = {}, {}

    def rows_piece(k):
        return lambda owner: xrows.at[owner, tp_peer[k]]

    def down_piece(k):
        return lambda owner: down_all.at[
            pl.ds(pl.multiple_of(owner * flat, flat), flat), columns(tp_peer[k])
        ]

    pending = []

    def advance(relay, lag):
        pending.append(relay)
        while len(pending) > lag:
            pending.pop(0)()

    own_rows.wait()
    for k in [0, 1] + near[:-1]:
        if k > 0:
            rows_copy[k].wait_recv()
        own, relay = spread(fx, k, rows_piece(k), fx_s, fx_r)
        own()
        if k in early:
            rows_copy[k].wait_send()
            w_copy[0, k].start()
        if k > 0:
            convert(1, k)
        if k in late:
            rows_copy[k].wait_send()
            w_copy[1, k].start()
        advance(relay, 1)
    for k in late:
        convert(2, k)
    for k in [0, 1] + [k for k in early if k != 1]:
        if k > 0:
            w_copy[2, k].wait_recv()
        own, relay = spread(dx, k, down_piece(k), dx_s, dx_r)
        own()
        if k > 0:
            w_copy[2, k].wait_send()
            w_copy[1, k].start()
        advance(relay, 1)
    for k in late:
        w_copy[0, k].wait_send()
        w_copy[2, k].start()
    advance(lambda: None, 0)
    for k in range(tp_n):
        fx[k, 1].wait_recv()
        fx[k, 2].wait_recv()

    def pair_columns(pair):
        base = tp_peer[pair] - lax.rem(tp_peer[pair], 2)
        return pl.ds(pl.multiple_of(base * width, 2 * width), 2 * width)

    def pair_product(b, at):
        x = xrows[b, :, :, at].reshape(block, 2 * width)
        gate = lax.dot_general(x, gate_out[:, at], NT, preferred_element_type=jnp.float32)
        up = lax.dot_general(x, up_out[:, at], NT, preferred_element_type=jnp.float32)
        return gate, up

    for pair in pairs[:-1]:
        for k in (pair, pair + 1):
            if k > 0:
                w_copy[0, k].wait_recv()
                w_copy[1, k].wait_recv()
        at = pair_columns(pair)

        @pl.loop(0, fs_n)
        def _(b):
            gate, up = pair_product(b, at)
            if pair > 0:
                gate = gate + acc[b, :, :flat]
                up = up + acc[b, :, flat:]
            acc[b, :, :flat] = gate
            acc[b, :, flat:] = up

    for k in (pairs[-1], pairs[-1] + 1):
        w_copy[0, k].wait_recv()
        w_copy[1, k].wait_recv()
    h_copy = {}
    own_units = pl.ds(pl.multiple_of(f * flat, flat), flat)
    for j in (3, 1, 2, 0):
        b = fs_peer[j]
        gate, up = pair_product(b, pair_columns(pairs[-1]))
        gate = gate + acc[b, :, :flat]
        up = up + acc[b, :, flat:]
        active = gate / (1.0 + jnp.exp(-gate)) * up
        route = xrows[b, :, :, model:].reshape(block, LANES).astype(jnp.float32)
        for e in range(experts):
            at = slice(e * units, (e + 1) * units)
            hid[j, :, at] = (route[:, e : e + 1] * active[:, at]).astype(jnp.bfloat16)
        if j > 0:
            h_copy[j] = remote(
                hid.at[j], hcat.at[:, own_units], h_s.at[j], h_r.at[j], b, t
            )
            h_copy[j].start()
        else:
            hcat[:, own_units] = hid[j]
    for copy in h_copy.values():
        copy.wait_recv()

    ret_copy = {}

    def give_back(pair):
        for k in (pair, pair + 1):
            dx[k, 1].wait_recv()
            dx[k, 2].wait_recv()
        at = pair_columns(pair)
        total = jnp.dot(hcat[...], down_all[:, at], preferred_element_type=jnp.float32)
        rsum[pair // 2] = total.astype(jnp.bfloat16).reshape(tp_n, cap, 2 * width)
        for k in near:
            ret_copy[pair, k] = remote(
                rsum.at[pair // 2, tp_peer[k]], ret.at[t, :, at],
                ret_s.at[pair // 2, k], ret_r.at[pair // 2, k], f, tp_peer[k],
            )
            ret_copy[pair, k].start()
        ret[t, :, at] = rsum[pair // 2, t]

    order = [pair for pair in pairs if pair not in late]
    give_back(order[0])
    for k in late:
        w_copy[2, k].wait_recv()
        own, relay = spread(dx, k, down_piece(k), dx_s, dx_r)
        own()
        advance(relay, 2)
    down_kept = pltpu.make_async_copy(down_all.at[own_down], down_out, loc.at[1])
    down_kept.start()
    for pair in order[1:]:
        give_back(pair)
        if pending:
            pending.pop(0)()
    advance(lambda: None, 0)
    give_back(late[0])

    down_kept.wait()
    for copy in ret_copy.values():
        copy.wait_recv()
    for (m, k), copy in w_copy.items():
        if (m == 2 and k in early) or (m == 0 and k in late):
            continue
        copy.wait_send()
    for group in (fx, dx, h_copy, ret_copy):
        for copy in group.values():
            copy.wait_send()


def finish_kernel(
    gate_in, up_in, down_in, ret_ref, placing_ref,
    gate_out, up_out, down_out, mixed_ref, sems,
):
    copies = [
        pltpu.make_async_copy(src, dst, sems.at[i])
        for i, (src, dst) in enumerate(((gate_in, gate_out), (up_in, up_out), (down_in, down_out)))
    ]
    for copy in copies:
        copy.start()
    mixed_ref[...] = lax.dot_general(
        placing_ref[...], ret_ref[...], TN, preferred_element_type=jnp.float32
    ).astype(jnp.bfloat16)
    for copy in copies:
        copy.wait()


def fused_device(fs_n, gate, up, down, prompt, norm_gain, group_pick, route_weight, capacity):
    tp_n, experts, units, width = gate.shape
    tokens, model = prompt.shape
    flat = experts * units
    block = tp_n * capacity
    bf16, f32 = jnp.bfloat16, jnp.float32
    dma = pltpu.SemaphoreType.DMA
    vmem = pl.BlockSpec(memory_space=pltpu.VMEM)
    hbm = pl.BlockSpec(memory_space=pltpu.HBM)
    anywhere = pl.BlockSpec(memory_space=pl.ANY)
    dims = (fs_n, tp_n, experts, units, width, model, capacity)
    served = jax.ShapeDtypeStruct((flat, model), bf16)
    gate_v, up_v, down_v, ret, placing = pl.pallas_call(
        functools.partial(exchange_kernel, dims),
        out_shape=(
            served,
            served,
            served,
            jax.ShapeDtypeStruct((tp_n, capacity, model), bf16),
            jax.ShapeDtypeStruct((block, tokens), bf16),
        ),
        in_specs=[hbm] * 7,
        out_specs=(vmem,) * 5,
        scratch_shapes=[
            pltpu.VMEM((1, width), f32),
            pltpu.VMEM((1, tokens), jnp.int32),
            pltpu.VMEM((experts, tokens), bf16),
            pltpu.VMEM((fs_n * flat, model), bf16),
            pltpu.VMEM((tokens, model), bf16),
            pltpu.VMEM((3, tp_n, flat, width), f32),
            pltpu.VMEM((3, tp_n, flat, width), bf16),
            pltpu.VMEM((tp_n, capacity, model + LANES), bf16),
            pltpu.VMEM((fs_n, tp_n, capacity, model + LANES), bf16),
            pltpu.VMEM((fs_n, block, 2 * flat), f32),
            pltpu.VMEM((fs_n, block, flat), bf16),
            pltpu.VMEM((block, fs_n * flat), bf16),
            pltpu.VMEM((tp_n // 2, tp_n, capacity, 2 * width), bf16),
            pltpu.VMEM((LANES, tokens), bf16),
            dma((4, tp_n)),
            dma((tp_n,)), dma((tp_n,)),
            dma((3, tp_n)), dma((3, tp_n)),
            dma((tp_n, 3)), dma((tp_n, 3)),
            dma((tp_n, 3)), dma((tp_n, 3)),
            dma((fs_n,)), dma((fs_n,)),
            dma((tp_n // 2, tp_n)), dma((tp_n // 2, tp_n)),
            dma((2,)),
        ],
        compiler_params=pltpu.CompilerParams(
            collective_id=0, has_side_effects=True, vmem_limit_bytes=44 * 2**20
        ),
    )(
        *(
            pltpu.with_memory_space_constraint(value, pltpu.HBM)
            for value in (
                prompt,
                norm_gain.reshape(1, width),
                gate.reshape(tp_n, flat, width),
                up.reshape(tp_n, flat, width),
                down.reshape(tp_n, flat, width),
                group_pick.reshape(1, tokens),
                route_weight.T,
            )
        )
    )
    gate_serve, up_serve, down_serve, mixed = pl.pallas_call(
        finish_kernel,
        out_shape=(served, served, served, jax.ShapeDtypeStruct((tokens, model), bf16)),
        in_specs=[anywhere, anywhere, anywhere, vmem, vmem],
        out_specs=(hbm, hbm, hbm, vmem),
        scratch_shapes=[dma((3,))],
        compiler_params=pltpu.CompilerParams(vmem_limit_bytes=16 * 2**20),
    )(gate_v, up_v, down_v, ret.reshape(block, model), placing)
    shape = (1, experts, units, model)
    return gate_serve.reshape(shape), up_serve.reshape(shape), down_serve.reshape(shape), mixed


def per_device(prompt, norm_gain, gate_master, up_master, down_master, group_pick, route_weight):
    group_total = lax.axis_size("tp")
    fs_n = lax.axis_size("fs")
    tok_count = prompt.shape[0]
    capacity = 2 * tok_count // group_total
    slot_total = group_total * capacity
    width, units = gate_master.shape[3], gate_master.shape[2]
    small = group_total == 8 and fs_n == 4
    if small and width % (2 * LANES) == 0 and units % LANES == 0 and capacity % 16 == 0:
        return fused_device(
            fs_n, gate_master, up_master, down_master,
            prompt, norm_gain, group_pick, route_weight, capacity,
        )
    gate_local = (gate_master * norm_gain).astype(jnp.bfloat16)
    up_local = (up_master * norm_gain).astype(jnp.bfloat16)
    down_local = down_master.astype(jnp.bfloat16)
    values = prompt.astype(jnp.float32)
    normed = (values * lax.rsqrt(jnp.mean(values * values, axis=1, keepdims=True) + EPS)).astype(
        jnp.bfloat16
    )
    chosen = group_pick[:, 0]
    member = (chosen[:, None] == jnp.arange(group_total, dtype=jnp.int32)[None, :]).astype(
        jnp.int32
    )
    slot_rank = jnp.sum(jnp.cumsum(member, axis=0) * member, axis=1) - 1
    target = chosen * capacity + slot_rank
    placing = (jnp.arange(slot_total, dtype=jnp.int32)[:, None] == target[None, :]).astype(
        jnp.bfloat16
    )
    gate_serve, up_serve, down_serve = (
        lax.all_to_all(gate_local, "tp", split_axis=0, concat_axis=3, tiled=True),
        lax.all_to_all(up_local, "tp", split_axis=0, concat_axis=3, tiled=True),
        lax.all_to_all(down_local, "tp", split_axis=0, concat_axis=3, tiled=True),
    )
    send_rows = jnp.dot(placing, normed, preferred_element_type=jnp.float32).astype(jnp.bfloat16)
    send_weights = jnp.dot(placing, route_weight, preferred_element_type=jnp.float32).astype(
        jnp.bfloat16
    )
    got_rows, got_weights = (
        lax.all_to_all(
            send_rows.reshape(group_total, capacity, -1),
            "tp",
            split_axis=0,
            concat_axis=0,
            tiled=True,
        ),
        lax.all_to_all(
            send_weights.reshape(group_total, capacity, -1),
            "tp",
            split_axis=0,
            concat_axis=0,
            tiled=True,
        ),
    )
    group_rows = got_rows.reshape(slot_total, -1)
    weights = got_weights.reshape(slot_total, -1)
    gathered = (
        lax.all_gather(gate_serve, "fs", axis=2, tiled=True),
        lax.all_gather(up_serve, "fs", axis=2, tiled=True),
        lax.all_gather(down_serve, "fs", axis=2, tiled=True),
    )
    summed = expert_rows(group_rows, weights, gathered)
    result = summed.astype(jnp.bfloat16).reshape(group_total, capacity, -1)
    returned = lax.all_to_all(result, "tp", split_axis=0, concat_axis=0, tiled=True)
    mixed = jnp.einsum(
        "st,sd->td", placing, returned.reshape(slot_total, -1), preferred_element_type=jnp.float32
    ).astype(jnp.bfloat16)
    return (gate_serve, up_serve, down_serve, mixed)


def solution(mesh):
    placed = (
        P(("fs", "tp"), None),
        P("tp"),
        P(None, None, "fs", "tp"),
        P(None, None, "fs", "tp"),
        P(None, None, "fs", "tp"),
        P(("fs", "tp"), None),
        P(("fs", "tp"), None),
    )
    return jax.shard_map(
        per_device,
        mesh=mesh,
        in_specs=placed,
        out_specs=(
            P("tp", None, "fs", None),
            P("tp", None, "fs", None),
            P("tp", None, "fs", None),
            P(("fs", "tp"), None),
        ),
        check_vma=False,
    )
```

```python
import functools

import jax
import jax.numpy as jnp
from jax import lax
from jax.experimental import pallas as pl
from jax.experimental.pallas import tpu as pltpu
from jax.sharding import PartitionSpec as P

EPS = 1e-06
MESH = pl.DeviceIdType.MESH
LANES = 128
NT = (((1,), (1,)), ((), ()))
TN = (((0,), (0,)), ((), ()))


def expert_rows(group_rows, weights, pieces):
    gate_piece, up_piece, down_piece = pieces
    expert_count = gate_piece.shape[1]
    unit_count = gate_piece.shape[2]
    model_width = gate_piece.shape[3]
    row_count = group_rows.shape[0]
    gate_matrix = gate_piece.reshape(expert_count * unit_count, model_width)
    up_matrix = up_piece.reshape(expert_count * unit_count, model_width)
    down_matrix = down_piece.reshape(expert_count * unit_count, model_width)
    gate_pre = jnp.einsum("sd,hd->sh", group_rows, gate_matrix, preferred_element_type=jnp.float32)
    up_pre = jnp.einsum("sd,hd->sh", group_rows, up_matrix, preferred_element_type=jnp.float32)
    active = (jax.nn.silu(gate_pre) * up_pre).reshape(row_count, expert_count, unit_count)
    hidden = (weights.astype(jnp.float32)[:, :, None] * active).reshape(
        row_count, expert_count * unit_count
    )
    hidden = hidden.astype(jnp.bfloat16)
    return jnp.dot(hidden, down_matrix, preferred_element_type=jnp.float32)


def flipped(index, mask, size):
    total, bit = 0, 1
    while bit < size:
        digit = lax.rem(lax.div(index, bit), 2)
        total = total + bit * ((1 - digit) if mask & bit else digit)
        bit *= 2
    return total


class Transfer:
    def __init__(self, copy, log):
        self.copy, self.log, self.sent, self.got = copy, log, False, False

    def start(self):
        self.log.append(self)
        self.copy.start()

    def wait_send(self):
        if not self.sent:
            self.sent = True
            self.copy.wait_send()

    def wait_recv(self):
        if not self.got:
            self.got = True
            self.copy.wait_recv()


def exchange_kernel(
    dims,
    prompt_in, gain_in, gate_in, up_in, down_in, pick_in, route_in,
    gate_out, up_out, down_out, ret, placing_ref,
    gain_ref, pick_ref, route_ref, down_all, prompt, stage, wsend, rows, xrows, acc, hid, hcat,
    rsum, route_send, route_all,
    load, rows_s, rows_r, w_s, w_r, fx_s, fx_r, dx_s, dx_r, h_s, h_r, ret_s, ret_r,
    rt_s, rt_r, rx_s, rx_r, loc,
):
    fs_n, tp_n, experts, units, width, model, cap = dims
    flat, block, tokens = experts * units, tp_n * cap, prompt.shape[0]
    f = lax.axis_index("fs")
    t = lax.axis_index("tp")
    tp_peer = [flipped(t, k, tp_n) for k in range(tp_n)]
    fs_peer = [flipped(f, j, fs_n) for j in range(fs_n)]

    near = list(range(2, tp_n)) + [1]
    late = list(range(tp_n // 2, tp_n))
    far_first = late + [k for k in near if k not in late]
    fill = tp_n - 2
    pairs = list(range(0, tp_n, 2))
    gate_m, up_m, down_m, rows_m = 0, 1, 2, 3
    plan = {}
    for k in near:
        if k in late:
            plan[k] = [rows_m, gate_m, up_m, down_m]
        else:
            plan[k] = [rows_m, down_m, gate_m, up_m]
    plan[fill] = [gate_m, rows_m, up_m, down_m]
    plan[1] = [down_m, rows_m, gate_m, up_m]

    sources = (gate_in, up_in, down_in)
    loads = {}

    def load_weight(m, k):
        loads[m, k] = pltpu.make_async_copy(
            sources[m].at[tp_peer[k]], stage.at[m, k], load.at[m, k]
        )
        loads[m, k].start()

    small_loads = [
        pltpu.make_async_copy(src, dst, load.at[3, 1 + i])
        for i, (src, dst) in enumerate(
            ((gain_in, gain_ref), (pick_in, pick_ref), (route_in, route_ref))
        )
    ]
    for copy in small_loads:
        copy.start()
    load_weight(gate_m, fill)
    load_weight(down_m, 0)
    load_weight(down_m, 1)
    prompt_load = pltpu.make_async_copy(prompt_in, prompt, load.at[3, 0])
    prompt_load.start()
    for m in (down_m, gate_m, up_m):
        for k in range(tp_n):
            if (m, k) not in loads:
                load_weight(m, k)

    started = []
    barrier = pltpu.get_barrier_semaphore()
    for k in range(1, tp_n):
        pl.semaphore_signal(barrier, inc=1, device_id=(f, tp_peer[k]), device_id_type=MESH)
    for j in range(1, fs_n):
        pl.semaphore_signal(barrier, inc=1, device_id=(fs_peer[j], t), device_id_type=MESH)

    def columns(index):
        return pl.ds(pl.multiple_of(index * width, width), width)

    def own_rows_of(owner):
        return pl.ds(pl.multiple_of(owner * flat, flat), flat)

    def remote(src, dst, send, recv, fs_to, tp_to):
        copy = pltpu.make_async_remote_copy(
            src_ref=src, dst_ref=dst, send_sem=send, recv_sem=recv,
            device_id=(fs_to, tp_to), device_id_type=MESH,
        )
        return Transfer(copy, started)

    copies = {}
    landing = (
        gate_out.at[:, columns(t)],
        up_out.at[:, columns(t)],
        down_all.at[own_rows_of(f), columns(t)],
    )
    for k in near:
        for m in (gate_m, up_m, down_m):
            copies[m, k] = remote(
                wsend.at[m, k], landing[m], w_s.at[m, k], w_r.at[m, k], f, tp_peer[k]
            )
        copies[rows_m, k] = remote(
            rows.at[tp_peer[k]], xrows.at[f, t], rows_s.at[k], rows_r.at[k], f, tp_peer[k]
        )

    def convert(m, k):
        loads[m, k].wait()
        value = stage[m, k]
        if m != down_m:
            value = value * gain_ref[...]
        value = value.astype(jnp.bfloat16)
        if k > 0:
            wsend[m, k] = value
        elif m == down_m:
            down_all[own_rows_of(f), columns(t)] = value
        else:
            (gate_out, up_out)[m][:, columns(t)] = value

    def spread(log, k, piece, send, recv):
        first, second = (1, 2) if (k // 2 + k) % 2 == 0 else (2, 1)

        def go(slot, owner, to):
            ref = piece(owner)
            log[k, slot] = remote(ref, ref, send.at[k, slot], recv.at[k, slot], fs_peer[to], t)
            log[k, slot].start()

        go(0, f, first)
        go(1, f, second)

        def relay():
            log[k, 0].wait_recv()
            go(2, fs_peer[first], second)

        return relay

    fx, dx = {}, {}

    def spread_rows(k):
        return spread(fx, k, lambda owner: xrows.at[owner, tp_peer[k]], fx_s, fx_r)

    def spread_down(k):
        return spread(
            dx, k, lambda owner: down_all.at[own_rows_of(owner), columns(tp_peer[k])], dx_s, dx_r
        )

    pending = []

    def advance(lag, relay=None):
        if relay is not None:
            pending.append(relay)
        while len(pending) > lag:
            pending.pop(0)()

    for copy in small_loads:
        copy.wait()
    convert(gate_m, fill)
    convert(down_m, 1)
    convert(down_m, 0)
    pick = pick_ref[...].astype(jnp.float32)
    group_id = lax.broadcasted_iota(jnp.int32, (tp_n, tokens), 0).astype(jnp.float32)
    member = jnp.where(group_id == pick, 1.0, 0.0)
    ahead = jnp.where(
        lax.broadcasted_iota(jnp.int32, (tokens, tokens), 0)
        <= lax.broadcasted_iota(jnp.int32, (tokens, tokens), 1),
        1.0, 0.0,
    ).astype(jnp.bfloat16)
    count = jnp.dot(member.astype(jnp.bfloat16), ahead, preferred_element_type=jnp.float32)
    rank = jnp.sum(member * count, axis=0, keepdims=True) - 1.0
    target = pick * cap + rank
    slot = lax.broadcasted_iota(jnp.int32, (block, tokens), 0).astype(jnp.float32)
    placing = jnp.where(slot == target, 1.0, 0.0).astype(jnp.bfloat16)
    placing_ref[...] = placing

    pl.semaphore_wait(barrier, tp_n - 1 + fs_n - 1)
    copies[gate_m, fill].start()
    copies[down_m, 1].start()
    advance(1, spread_down(0))

    prompt_load.wait()
    values = prompt[...].astype(jnp.float32)
    scale = lax.rsqrt(jnp.mean(values * values, axis=1, keepdims=True) + EPS)
    normed = (values * scale).astype(jnp.bfloat16)
    rows[...] = (
        jnp.dot(placing, normed, preferred_element_type=jnp.float32)
        .astype(jnp.bfloat16)
        .reshape(tp_n, cap, model)
    )
    for k in near:
        copies[rows_m, k].start()
    own_rows = pltpu.make_async_copy(rows.at[t], xrows.at[f, t], loc.at[0])
    own_rows.start()
    route_send[...] = jnp.zeros_like(route_send)
    for g in range(tp_n):
        route_send[g, :, :cap] = lax.dot_general(
            route_ref[...], placing_ref[g * cap : (g + 1) * cap, :], NT,
            preferred_element_type=jnp.float32,
        )
    route_copy = {}
    for k in near:
        route_copy[k] = remote(
            route_send.at[tp_peer[k]], route_all.at[f, t], rt_s.at[k], rt_r.at[k], f, tp_peer[k]
        )
        route_copy[k].start()
    route_all[f, t] = route_send[t]

    for k in near:
        m = plan[k][1]
        if k != 1 and m != rows_m:
            convert(m, k)
            copies[m, k].start()
    for k in near:
        m = plan[k][2]
        convert(m, k)
    convert(gate_m, 0)
    convert(up_m, 0)

    copies[down_m, 1].wait_recv()
    advance(1, spread_down(1))
    own_rows.wait()
    for k in [0, 1] + near[:-1]:
        if k > 0:
            copies[rows_m, k].wait_recv()
        advance(1, spread_rows(k))
        if k > 0:
            copies[plan[k][0], k].wait_send()
            copies[plan[k][2], k].start()
            convert(plan[k][3], k)
    for k in range(2, tp_n):
        if k not in late:
            copies[down_m, k].wait_recv()
            advance(1, spread_down(k))
    for k in near:
        copies[plan[k][1], k].wait_send()
        if k not in late:
            copies[plan[k][3], k].start()
    advance(0)
    for k in near:
        route_copy[k].wait_recv()
    route_spread = []
    for j in range(1, fs_n):
        copy = remote(
            route_all.at[f], route_all.at[f], rx_s.at[j], rx_r.at[j], fs_peer[j], t
        )
        copy.start()
        route_spread.append(copy)
    for k in range(tp_n):
        fx[k, 1].wait_recv()
        fx[k, 2].wait_recv()
    for copy in route_spread:
        copy.wait_recv()

    def pair_columns(pair):
        base = tp_peer[pair] - lax.rem(tp_peer[pair], 2)
        return pl.ds(pl.multiple_of(base * width, 2 * width), 2 * width)

    def pair_product(b, at):
        x = xrows[b, :, :, at].reshape(block, 2 * width)
        gate = lax.dot_general(x, gate_out[:, at], NT, preferred_element_type=jnp.float32)
        up = lax.dot_general(x, up_out[:, at], NT, preferred_element_type=jnp.float32)
        return gate, up

    for pair in pairs[:-1]:
        if pair == late[0]:
            for k in late:
                copies[up_m, k].wait_send()
                copies[down_m, k].start()
        for k in (pair, pair + 1):
            if k > 0:
                copies[gate_m, k].wait_recv()
                copies[up_m, k].wait_recv()
        at = pair_columns(pair)

        @pl.loop(0, fs_n)
        def _(b):
            gate, up = pair_product(b, at)
            if pair > 0:
                gate = gate + acc[b, :, :flat]
                up = up + acc[b, :, flat:]
            acc[b, :, :flat] = gate
            acc[b, :, flat:] = up

    for k in (pairs[-1], pairs[-1] + 1):
        copies[gate_m, k].wait_recv()
        copies[up_m, k].wait_recv()
    h_copy = {}
    for j in (3, 1, 2, 0):
        b = fs_peer[j]
        gate, up = pair_product(b, pair_columns(pairs[-1]))
        gate = gate + acc[b, :, :flat]
        up = up + acc[b, :, flat:]
        active = gate / (1.0 + jnp.exp(-gate)) * up
        for s in range(tp_n):
            line = slice(s * cap, (s + 1) * cap)
            route = jnp.transpose(route_all[b, s])
            for e in range(experts):
                at = slice(e * units, (e + 1) * units)
                hid[j, line, at] = (route[:cap, e : e + 1] * active[line, at]).astype(jnp.bfloat16)
        if j > 0:
            h_copy[j] = remote(
                hid.at[j], hcat.at[:, own_rows_of(f)], h_s.at[j], h_r.at[j], b, t
            )
            h_copy[j].start()
        else:
            hcat[:, own_rows_of(f)] = hid[j]

    ret_copy = {}

    def give_back(pair):
        for k in (pair, pair + 1):
            dx[k, 1].wait_recv()
            dx[k, 2].wait_recv()
        at = pair_columns(pair)
        total = jnp.dot(hcat[...], down_all[:, at], preferred_element_type=jnp.float32)
        rsum[pair // 2] = total.astype(jnp.bfloat16).reshape(tp_n, cap, 2 * width)
        for k in far_first:
            ret_copy[pair, k] = remote(
                rsum.at[pair // 2, tp_peer[k]], ret.at[t, :, at],
                ret_s.at[pair // 2, k], ret_r.at[pair // 2, k], f, tp_peer[k],
            )
            ret_copy[pair, k].start()
        ret[t, :, at] = rsum[pair // 2, t]

    for k in late[:2]:
        copies[down_m, k].wait_recv()
        advance(1, spread_down(k))
    for copy in h_copy.values():
        copy.wait_recv()
    for pair in pairs:
        if pair not in late:
            give_back(pair)
    for k in late[2:]:
        copies[down_m, k].wait_recv()
        advance(1, spread_down(k))
    advance(0)
    down_kept = pltpu.make_async_copy(down_all.at[own_rows_of(f)], down_out, loc.at[1])
    down_kept.start()
    for pair in pairs:
        if pair in late:
            give_back(pair)

    down_kept.wait()
    for copy in ret_copy.values():
        copy.wait_recv()
    for copy in started:
        copy.wait_send()


def finish_kernel(
    gate_in, up_in, down_in, ret_ref, placing_ref,
    gate_out, up_out, down_out, mixed_out, mixed, sems, mixed_sems,
):
    copies = [
        pltpu.make_async_copy(src, dst, sems.at[i])
        for i, (src, dst) in enumerate(((gate_in, gate_out), (up_in, up_out), (down_in, down_out)))
    ]
    for copy in copies:
        copy.start()
    parts = mixed_sems.shape[0]
    step = mixed.shape[1] // parts
    for i in range(parts):
        at = slice(i * step, (i + 1) * step)
        mixed[:, at] = lax.dot_general(
            placing_ref[...], ret_ref[:, at], TN, preferred_element_type=jnp.float32
        ).astype(jnp.bfloat16)
        copy = pltpu.make_async_copy(mixed.at[:, at], mixed_out.at[:, at], mixed_sems.at[i])
        copy.start()
        copies.append(copy)
    for copy in copies:
        copy.wait()


def fused_device(fs_n, gate, up, down, prompt, norm_gain, group_pick, route_weight, capacity):
    tp_n, experts, units, width = gate.shape
    tokens, model = prompt.shape
    flat = experts * units
    block = tp_n * capacity
    bf16, f32 = jnp.bfloat16, jnp.float32
    dma = pltpu.SemaphoreType.DMA
    vmem = pl.BlockSpec(memory_space=pltpu.VMEM)
    hbm = pl.BlockSpec(memory_space=pltpu.HBM)
    anywhere = pl.BlockSpec(memory_space=pl.ANY)
    dims = (fs_n, tp_n, experts, units, width, model, capacity)
    served = jax.ShapeDtypeStruct((flat, model), bf16)
    gate_v, up_v, down_v, ret, placing = pl.pallas_call(
        functools.partial(exchange_kernel, dims),
        out_shape=(
            served,
            served,
            served,
            jax.ShapeDtypeStruct((tp_n, capacity, model), bf16),
            jax.ShapeDtypeStruct((block, tokens), bf16),
        ),
        in_specs=[hbm] * 7,
        out_specs=(vmem,) * 5,
        scratch_shapes=[
            pltpu.VMEM((1, width), f32),
            pltpu.VMEM((1, tokens), jnp.int32),
            pltpu.VMEM((experts, tokens), bf16),
            pltpu.VMEM((fs_n * flat, model), bf16),
            pltpu.VMEM((tokens, model), bf16),
            pltpu.VMEM((3, tp_n, flat, width), f32),
            pltpu.VMEM((3, tp_n, flat, width), bf16),
            pltpu.VMEM((tp_n, capacity, model), bf16),
            pltpu.VMEM((fs_n, tp_n, capacity, model), bf16),
            pltpu.VMEM((fs_n, block, 2 * flat), f32),
            pltpu.VMEM((fs_n, block, flat), bf16),
            pltpu.VMEM((block, fs_n * flat), bf16),
            pltpu.VMEM((tp_n // 2, tp_n, capacity, 2 * width), bf16),
            pltpu.VMEM((tp_n, experts, LANES), f32),
            pltpu.VMEM((fs_n, tp_n, experts, LANES), f32),
            dma((4, tp_n)),
            dma((tp_n,)), dma((tp_n,)),
            dma((3, tp_n)), dma((3, tp_n)),
            dma((tp_n, 3)), dma((tp_n, 3)),
            dma((tp_n, 3)), dma((tp_n, 3)),
            dma((fs_n,)), dma((fs_n,)),
            dma((tp_n // 2, tp_n)), dma((tp_n // 2, tp_n)),
            dma((tp_n,)), dma((tp_n,)),
            dma((fs_n,)), dma((fs_n,)),
            dma((2,)),
        ],
        compiler_params=pltpu.CompilerParams(
            collective_id=0, has_side_effects=True, vmem_limit_bytes=44 * 2**20
        ),
    )(
        *(
            pltpu.with_memory_space_constraint(value, pltpu.HBM)
            for value in (
                prompt,
                norm_gain.reshape(1, width),
                gate.reshape(tp_n, flat, width),
                up.reshape(tp_n, flat, width),
                down.reshape(tp_n, flat, width),
                group_pick.reshape(1, tokens),
                route_weight.T,
            )
        )
    )
    gate_serve, up_serve, down_serve, mixed = pl.pallas_call(
        finish_kernel,
        out_shape=(served, served, served, jax.ShapeDtypeStruct((tokens, model), bf16)),
        in_specs=[anywhere, anywhere, anywhere, vmem, vmem],
        out_specs=(hbm,) * 4,
        scratch_shapes=[pltpu.VMEM((tokens, model), bf16), dma((3,)), dma((4,))],
        compiler_params=pltpu.CompilerParams(vmem_limit_bytes=16 * 2**20),
    )(gate_v, up_v, down_v, ret.reshape(block, model), placing)
    shape = (1, experts, units, model)
    return gate_serve.reshape(shape), up_serve.reshape(shape), down_serve.reshape(shape), mixed


def per_device(prompt, norm_gain, gate_master, up_master, down_master, group_pick, route_weight):
    group_total = lax.axis_size("tp")
    fs_n = lax.axis_size("fs")
    tok_count = prompt.shape[0]
    capacity = 2 * tok_count // group_total
    slot_total = group_total * capacity
    width, units = gate_master.shape[3], gate_master.shape[2]
    small = group_total == 8 and fs_n == 4
    if small and width % (2 * LANES) == 0 and units % LANES == 0 and capacity % 16 == 0:
        return fused_device(
            fs_n, gate_master, up_master, down_master,
            prompt, norm_gain, group_pick, route_weight, capacity,
        )
    gate_local = (gate_master * norm_gain).astype(jnp.bfloat16)
    up_local = (up_master * norm_gain).astype(jnp.bfloat16)
    down_local = down_master.astype(jnp.bfloat16)
    values = prompt.astype(jnp.float32)
    normed = (values * lax.rsqrt(jnp.mean(values * values, axis=1, keepdims=True) + EPS)).astype(
        jnp.bfloat16
    )
    chosen = group_pick[:, 0]
    member = (chosen[:, None] == jnp.arange(group_total, dtype=jnp.int32)[None, :]).astype(
        jnp.int32
    )
    slot_rank = jnp.sum(jnp.cumsum(member, axis=0) * member, axis=1) - 1
    target = chosen * capacity + slot_rank
    placing = (jnp.arange(slot_total, dtype=jnp.int32)[:, None] == target[None, :]).astype(
        jnp.bfloat16
    )
    gate_serve, up_serve, down_serve = (
        lax.all_to_all(gate_local, "tp", split_axis=0, concat_axis=3, tiled=True),
        lax.all_to_all(up_local, "tp", split_axis=0, concat_axis=3, tiled=True),
        lax.all_to_all(down_local, "tp", split_axis=0, concat_axis=3, tiled=True),
    )
    send_rows = jnp.dot(placing, normed, preferred_element_type=jnp.float32).astype(jnp.bfloat16)
    send_weights = jnp.dot(placing, route_weight, preferred_element_type=jnp.float32).astype(
        jnp.bfloat16
    )
    got_rows, got_weights = (
        lax.all_to_all(
            send_rows.reshape(group_total, capacity, -1),
            "tp",
            split_axis=0,
            concat_axis=0,
            tiled=True,
        ),
        lax.all_to_all(
            send_weights.reshape(group_total, capacity, -1),
            "tp",
            split_axis=0,
            concat_axis=0,
            tiled=True,
        ),
    )
    group_rows = got_rows.reshape(slot_total, -1)
    weights = got_weights.reshape(slot_total, -1)
    gathered = (
        lax.all_gather(gate_serve, "fs", axis=2, tiled=True),
        lax.all_gather(up_serve, "fs", axis=2, tiled=True),
        lax.all_gather(down_serve, "fs", axis=2, tiled=True),
    )
    summed = expert_rows(group_rows, weights, gathered)
    result = summed.astype(jnp.bfloat16).reshape(group_total, capacity, -1)
    returned = lax.all_to_all(result, "tp", split_axis=0, concat_axis=0, tiled=True)
    mixed = jnp.einsum(
        "st,sd->td", placing, returned.reshape(slot_total, -1), preferred_element_type=jnp.float32
    ).astype(jnp.bfloat16)
    return (gate_serve, up_serve, down_serve, mixed)


def solution(mesh):
    placed = (
        P(("fs", "tp"), None),
        P("tp"),
        P(None, None, "fs", "tp"),
        P(None, None, "fs", "tp"),
        P(None, None, "fs", "tp"),
        P(("fs", "tp"), None),
        P(("fs", "tp"), None),
    )
    return jax.shard_map(
        per_device,
        mesh=mesh,
        in_specs=placed,
        out_specs=(
            P("tp", None, "fs", None),
            P("tp", None, "fs", None),
            P("tp", None, "fs", None),
            P(("fs", "tp"), None),
        ),
        check_vma=False,
    )
```

```python
import functools

import jax
import jax.numpy as jnp
from jax import lax
from jax.experimental import pallas as pl
from jax.experimental.pallas import tpu as pltpu
from jax.sharding import PartitionSpec as P

EPS = 1e-06
MESH = pl.DeviceIdType.MESH
LANES = 128
NT = (((1,), (1,)), ((), ()))
TN = (((0,), (0,)), ((), ()))


def expert_rows(group_rows, weights, pieces):
    gate_piece, up_piece, down_piece = pieces
    expert_count = gate_piece.shape[1]
    unit_count = gate_piece.shape[2]
    model_width = gate_piece.shape[3]
    row_count = group_rows.shape[0]
    gate_matrix = gate_piece.reshape(expert_count * unit_count, model_width)
    up_matrix = up_piece.reshape(expert_count * unit_count, model_width)
    down_matrix = down_piece.reshape(expert_count * unit_count, model_width)
    gate_pre = jnp.einsum("sd,hd->sh", group_rows, gate_matrix, preferred_element_type=jnp.float32)
    up_pre = jnp.einsum("sd,hd->sh", group_rows, up_matrix, preferred_element_type=jnp.float32)
    active = (jax.nn.silu(gate_pre) * up_pre).reshape(row_count, expert_count, unit_count)
    hidden = (weights.astype(jnp.float32)[:, :, None] * active).reshape(
        row_count, expert_count * unit_count
    )
    hidden = hidden.astype(jnp.bfloat16)
    return jnp.dot(hidden, down_matrix, preferred_element_type=jnp.float32)


def flipped(index, mask, size):
    total, bit = 0, 1
    while bit < size:
        digit = lax.rem(lax.div(index, bit), 2)
        total = total + bit * ((1 - digit) if mask & bit else digit)
        bit *= 2
    return total


class Transfer:
    def __init__(self, copy, log):
        self.copy, self.log, self.sent, self.got = copy, log, False, False

    def start(self):
        self.log.append(self)
        self.copy.start()

    def wait_send(self):
        if not self.sent:
            self.sent = True
            self.copy.wait_send()

    def wait_recv(self):
        if not self.got:
            self.got = True
            self.copy.wait_recv()


def exchange_kernel(
    dims,
    prompt_in, gain_in, gate_in, up_in, down_in, pick_in, route_in,
    gate_out, up_out, down_out, ret, placing_ref,
    gain_ref, pick_ref, route_ref, down_all, prompt, stage, wsend, rows, xrows, acc, hid, hcat,
    rsum, route_send, route_all,
    load, rows_s, rows_r, w_s, w_r, fx_s, fx_r, dx_s, dx_r, h_s, h_r, ret_s, ret_r,
    rt_s, rt_r, rx_s, rx_r, loc, ready,
):
    fs_n, tp_n, experts, units, width, model, cap = dims
    flat, block, tokens = experts * units, tp_n * cap, prompt.shape[0]
    f = lax.axis_index("fs")
    t = lax.axis_index("tp")
    tp_peer = [flipped(t, k, tp_n) for k in range(tp_n)]
    fs_peer = [flipped(f, j, fs_n) for j in range(fs_n)]

    near = list(range(2, tp_n)) + [1]
    late = list(range(tp_n // 2, tp_n))
    far_first = late + [k for k in near if k not in late]
    fill = [tp_n - 2, tp_n - 1]
    inner = lax.rem(lax.div(lax.div(t, 2) + 1, 2), 2)
    pairs = list(range(0, tp_n, 2))
    gate_m, up_m, down_m, rows_m = 0, 1, 2, 3
    plan = {}
    for k in near:
        if k in late:
            plan[k] = [rows_m, gate_m, up_m, down_m]
        else:
            plan[k] = [rows_m, down_m, gate_m, up_m]
    for k in fill:
        plan[k] = [gate_m, rows_m, up_m, down_m]
    plan[1] = [down_m, rows_m, gate_m, up_m]

    sources = (gate_in, up_in, down_in)
    loads = {}

    def load_weight(m, k):
        loads[m, k] = pltpu.make_async_copy(
            sources[m].at[tp_peer[k]], stage.at[m, k], load.at[m, k]
        )
        loads[m, k].start()

    small_loads = [
        pltpu.make_async_copy(src, dst, load.at[3, 1 + i])
        for i, (src, dst) in enumerate(
            ((gain_in, gain_ref), (pick_in, pick_ref), (route_in, route_ref))
        )
    ]
    for copy in small_loads:
        copy.start()
    for k in fill:
        load_weight(gate_m, k)
    load_weight(down_m, 0)
    load_weight(down_m, 1)
    prompt_load = pltpu.make_async_copy(prompt_in, prompt, load.at[3, 0])
    prompt_load.start()
    for m in (down_m, gate_m, up_m):
        for k in range(tp_n):
            if (m, k) not in loads:
                load_weight(m, k)

    started = []
    barrier = pltpu.get_barrier_semaphore()

    def greet(sem, fs_to, tp_to):
        pl.semaphore_signal(sem, inc=1, device_id=(fs_to, tp_to), device_id_type=MESH)

    for k in (2, 3, 1):
        greet(barrier, f, tp_peer[k])
    for j in (1, 2):
        greet(barrier, fs_peer[j], t)

    @pl.when(inner == 1)
    def _():
        for k in fill:
            greet(barrier, f, tp_peer[k])

    def columns(index):
        return pl.ds(pl.multiple_of(index * width, width), width)

    def own_rows_of(owner):
        return pl.ds(pl.multiple_of(owner * flat, flat), flat)

    def remote(src, dst, send, recv, fs_to, tp_to):
        copy = pltpu.make_async_remote_copy(
            src_ref=src, dst_ref=dst, send_sem=send, recv_sem=recv,
            device_id=(fs_to, tp_to), device_id_type=MESH,
        )
        return Transfer(copy, started)

    copies = {}
    landing = (
        gate_out.at[:, columns(t)],
        up_out.at[:, columns(t)],
        down_all.at[own_rows_of(f), columns(t)],
    )
    for k in near:
        for m in (gate_m, up_m, down_m):
            copies[m, k] = remote(
                wsend.at[m, k], landing[m], w_s.at[m, k], w_r.at[m, k], f, tp_peer[k]
            )
        copies[rows_m, k] = remote(
            rows.at[tp_peer[k]], xrows.at[f, t], rows_s.at[k], rows_r.at[k], f, tp_peer[k]
        )

    def convert(m, k):
        loads[m, k].wait()
        value = stage[m, k]
        if m != down_m:
            value = value * gain_ref[...]
        value = value.astype(jnp.bfloat16)
        if k > 0:
            wsend[m, k] = value
        elif m == down_m:
            down_all[own_rows_of(f), columns(t)] = value
        else:
            (gate_out, up_out)[m][:, columns(t)] = value

    def spread(log, k, piece, send, recv):
        first, second = (1, 2) if (k // 2 + k) % 2 == 0 else (2, 1)

        def go(slot, owner, to):
            ref = piece(owner)
            log[k, slot] = remote(ref, ref, send.at[k, slot], recv.at[k, slot], fs_peer[to], t)
            log[k, slot].start()

        go(0, f, first)
        go(1, f, second)

        def relay():
            log[k, 0].wait_recv()
            go(2, fs_peer[first], second)

        return relay

    fx, dx = {}, {}

    def spread_rows(k):
        return spread(fx, k, lambda owner: xrows.at[owner, tp_peer[k]], fx_s, fx_r)

    def spread_down(k):
        return spread(
            dx, k, lambda owner: down_all.at[own_rows_of(owner), columns(tp_peer[k])], dx_s, dx_r
        )

    pending = []

    def advance(lag, relay=None):
        if relay is not None:
            pending.append(relay)
        while len(pending) > lag:
            pending.pop(0)()

    for copy in small_loads:
        copy.wait()
    for k in fill:
        convert(gate_m, k)

    pl.semaphore_wait(barrier, 5 + 2 * inner)

    @pl.when(inner == 1)
    def _():
        greet(ready.at[0], f, tp_peer[fill[0]])
        greet(ready.at[0], f, tp_peer[2])
        for k in fill:
            copies[gate_m, k].start()

    convert(down_m, 1)
    convert(down_m, 0)
    copies[down_m, 1].start()
    advance(1, spread_down(0))

    pick = pick_ref[...].astype(jnp.float32)
    group_id = lax.broadcasted_iota(jnp.int32, (tp_n, tokens), 0).astype(jnp.float32)
    member = jnp.where(group_id == pick, 1.0, 0.0)
    ahead = jnp.where(
        lax.broadcasted_iota(jnp.int32, (tokens, tokens), 0)
        <= lax.broadcasted_iota(jnp.int32, (tokens, tokens), 1),
        1.0, 0.0,
    ).astype(jnp.bfloat16)
    count = jnp.dot(member.astype(jnp.bfloat16), ahead, preferred_element_type=jnp.float32)
    rank = jnp.sum(member * count, axis=0, keepdims=True) - 1.0
    target = pick * cap + rank
    slot = lax.broadcasted_iota(jnp.int32, (block, tokens), 0).astype(jnp.float32)
    placing = jnp.where(slot == target, 1.0, 0.0).astype(jnp.bfloat16)
    placing_ref[...] = placing

    @pl.when(inner == 1)
    def _():
        pl.semaphore_wait(ready.at[0], 1)
        greet(ready.at[1], f, tp_peer[2])

    prompt_load.wait()
    values = prompt[...].astype(jnp.float32)
    scale = lax.rsqrt(jnp.mean(values * values, axis=1, keepdims=True) + EPS)
    normed = (values * scale).astype(jnp.bfloat16)
    rows[...] = (
        jnp.dot(placing, normed, preferred_element_type=jnp.float32)
        .astype(jnp.bfloat16)
        .reshape(tp_n, cap, model)
    )
    for k in near:
        if k not in late:
            copies[rows_m, k].start()

    @pl.when(inner == 0)
    def _():
        pl.semaphore_wait(ready.at[0], 1)
        pl.semaphore_wait(ready.at[1], 1)
        for k in fill:
            copies[gate_m, k].start()

    for k in late:
        copies[rows_m, k].start()
    own_rows = pltpu.make_async_copy(rows.at[t], xrows.at[f, t], loc.at[0])
    own_rows.start()
    route_send[...] = jnp.zeros_like(route_send)
    for g in range(tp_n):
        route_send[g, :, :cap] = lax.dot_general(
            route_ref[...], placing_ref[g * cap : (g + 1) * cap, :], NT,
            preferred_element_type=jnp.float32,
        )
    route_copy = {}
    for k in near:
        route_copy[k] = remote(
            route_send.at[tp_peer[k]], route_all.at[f, t], rt_s.at[k], rt_r.at[k], f, tp_peer[k]
        )
        route_copy[k].start()
    route_all[f, t] = route_send[t]

    for k in near:
        m = plan[k][1]
        if k != 1 and m != rows_m:
            convert(m, k)
            copies[m, k].start()
    for k in near:
        m = plan[k][2]
        convert(m, k)
    convert(gate_m, 0)
    convert(up_m, 0)

    copies[down_m, 1].wait_recv()
    advance(1, spread_down(1))
    own_rows.wait()
    for k in [0, 1] + near[:-1]:
        if k > 0:
            copies[rows_m, k].wait_recv()
        advance(1, spread_rows(k))
        if k > 0:
            copies[plan[k][0], k].wait_send()
            copies[plan[k][2], k].start()
            convert(plan[k][3], k)
    for k in range(2, tp_n):
        if k not in late:
            copies[down_m, k].wait_recv()
            advance(1, spread_down(k))
    for k in near:
        copies[plan[k][1], k].wait_send()
        if k not in late:
            copies[plan[k][3], k].start()
    advance(0)
    for k in near:
        route_copy[k].wait_recv()
    route_spread = []
    for j in range(1, fs_n):
        copy = remote(
            route_all.at[f], route_all.at[f], rx_s.at[j], rx_r.at[j], fs_peer[j], t
        )
        copy.start()
        route_spread.append(copy)
    for k in range(tp_n):
        fx[k, 1].wait_recv()
        fx[k, 2].wait_recv()
    for copy in route_spread:
        copy.wait_recv()

    def pair_columns(pair):
        base = tp_peer[pair] - lax.rem(tp_peer[pair], 2)
        return pl.ds(pl.multiple_of(base * width, 2 * width), 2 * width)

    def pair_product(b, at):
        x = xrows[b, :, :, at].reshape(block, 2 * width)
        gate = lax.dot_general(x, gate_out[:, at], NT, preferred_element_type=jnp.float32)
        up = lax.dot_general(x, up_out[:, at], NT, preferred_element_type=jnp.float32)
        return gate, up

    for pair in pairs[:-1]:
        if pair == late[0]:
            for k in late:
                copies[up_m, k].wait_send()
                copies[down_m, k].start()
        for k in (pair, pair + 1):
            if k > 0:
                copies[gate_m, k].wait_recv()
                copies[up_m, k].wait_recv()
        at = pair_columns(pair)

        @pl.loop(0, fs_n)
        def _(b):
            gate, up = pair_product(b, at)
            if pair > 0:
                gate = gate + acc[b, :, :flat]
                up = up + acc[b, :, flat:]
            acc[b, :, :flat] = gate
            acc[b, :, flat:] = up

    for k in (pairs[-1], pairs[-1] + 1):
        copies[gate_m, k].wait_recv()
        copies[up_m, k].wait_recv()
    h_copy = {}
    for j in (3, 1, 2, 0):
        b = fs_peer[j]
        gate, up = pair_product(b, pair_columns(pairs[-1]))
        gate = gate + acc[b, :, :flat]
        up = up + acc[b, :, flat:]
        active = gate / (1.0 + jnp.exp(-gate)) * up
        for s in range(tp_n):
            line = slice(s * cap, (s + 1) * cap)
            route = jnp.transpose(route_all[b, s])
            for e in range(experts):
                at = slice(e * units, (e + 1) * units)
                hid[j, line, at] = (route[:cap, e : e + 1] * active[line, at]).astype(jnp.bfloat16)
        if j > 0:
            h_copy[j] = remote(
                hid.at[j], hcat.at[:, own_rows_of(f)], h_s.at[j], h_r.at[j], b, t
            )
            h_copy[j].start()
        else:
            hcat[:, own_rows_of(f)] = hid[j]

    ret_copy = {}

    def give_back(pair):
        for k in (pair, pair + 1):
            dx[k, 1].wait_recv()
            dx[k, 2].wait_recv()
        at, part = pair_columns(pair), lax.div(tp_peer[pair], 2)
        total = jnp.dot(hcat[...], down_all[:, at], preferred_element_type=jnp.float32)
        rsum[pair // 2] = total.astype(jnp.bfloat16).reshape(tp_n, cap, 2 * width)
        for k in far_first:
            ret_copy[pair, k] = remote(
                rsum.at[pair // 2, tp_peer[k]], ret.at[part, t],
                ret_s.at[pair // 2, k], ret_r.at[pair // 2, k], f, tp_peer[k],
            )
            ret_copy[pair, k].start()
        ret[part, t] = rsum[pair // 2, t]

    for k in late[:2]:
        copies[down_m, k].wait_recv()
        advance(1, spread_down(k))
    for copy in h_copy.values():
        copy.wait_recv()
    for pair in pairs:
        if pair not in late:
            give_back(pair)
    for k in late[2:]:
        copies[down_m, k].wait_recv()
        advance(1, spread_down(k))
    advance(0)
    down_kept = pltpu.make_async_copy(down_all.at[own_rows_of(f)], down_out, loc.at[1])
    down_kept.start()
    for pair in pairs:
        if pair in late:
            give_back(pair)

    down_kept.wait()
    for copy in ret_copy.values():
        copy.wait_recv()
    for copy in started:
        copy.wait_send()


def finish_kernel(
    gate_in, up_in, down_in, ret_ref, placing_ref,
    gate_out, up_out, down_out, mixed_out, mixed, sems, mixed_sems,
):
    copies = [
        pltpu.make_async_copy(src, dst, sems.at[i])
        for i, (src, dst) in enumerate(((gate_in, gate_out), (up_in, up_out), (down_in, down_out)))
    ]
    for copy in copies:
        copy.start()
    parts, _, step = ret_ref.shape
    for i in range(parts):
        at = slice(i * step, (i + 1) * step)
        mixed[:, at] = lax.dot_general(
            placing_ref[...], ret_ref[i], TN, preferred_element_type=jnp.float32
        ).astype(jnp.bfloat16)
        copy = pltpu.make_async_copy(mixed.at[:, at], mixed_out.at[:, at], mixed_sems.at[i])
        copy.start()
        copies.append(copy)
    for copy in copies:
        copy.wait()


def fused_device(fs_n, gate, up, down, prompt, norm_gain, group_pick, route_weight, capacity):
    tp_n, experts, units, width = gate.shape
    tokens, model = prompt.shape
    flat = experts * units
    block = tp_n * capacity
    bf16, f32 = jnp.bfloat16, jnp.float32
    dma = pltpu.SemaphoreType.DMA
    vmem = pl.BlockSpec(memory_space=pltpu.VMEM)
    hbm = pl.BlockSpec(memory_space=pltpu.HBM)
    anywhere = pl.BlockSpec(memory_space=pl.ANY)
    dims = (fs_n, tp_n, experts, units, width, model, capacity)
    served = jax.ShapeDtypeStruct((flat, model), bf16)
    gate_v, up_v, down_v, ret, placing = pl.pallas_call(
        functools.partial(exchange_kernel, dims),
        out_shape=(
            served,
            served,
            served,
            jax.ShapeDtypeStruct((tp_n // 2, tp_n, capacity, 2 * width), bf16),
            jax.ShapeDtypeStruct((block, tokens), bf16),
        ),
        in_specs=[hbm] * 7,
        out_specs=(vmem,) * 5,
        scratch_shapes=[
            pltpu.VMEM((1, width), f32),
            pltpu.VMEM((1, tokens), jnp.int32),
            pltpu.VMEM((experts, tokens), bf16),
            pltpu.VMEM((fs_n * flat, model), bf16),
            pltpu.VMEM((tokens, model), bf16),
            pltpu.VMEM((3, tp_n, flat, width), f32),
            pltpu.VMEM((3, tp_n, flat, width), bf16),
            pltpu.VMEM((tp_n, capacity, model), bf16),
            pltpu.VMEM((fs_n, tp_n, capacity, model), bf16),
            pltpu.VMEM((fs_n, block, 2 * flat), f32),
            pltpu.VMEM((fs_n, block, flat), bf16),
            pltpu.VMEM((block, fs_n * flat), bf16),
            pltpu.VMEM((tp_n // 2, tp_n, capacity, 2 * width), bf16),
            pltpu.VMEM((tp_n, experts, LANES), f32),
            pltpu.VMEM((fs_n, tp_n, experts, LANES), f32),
            dma((4, tp_n)),
            dma((tp_n,)), dma((tp_n,)),
            dma((3, tp_n)), dma((3, tp_n)),
            dma((tp_n, 3)), dma((tp_n, 3)),
            dma((tp_n, 3)), dma((tp_n, 3)),
            dma((fs_n,)), dma((fs_n,)),
            dma((tp_n // 2, tp_n)), dma((tp_n // 2, tp_n)),
            dma((tp_n,)), dma((tp_n,)),
            dma((fs_n,)), dma((fs_n,)),
            dma((2,)),
            pltpu.SemaphoreType.REGULAR((2,)),
        ],
        compiler_params=pltpu.CompilerParams(
            collective_id=0, has_side_effects=True, vmem_limit_bytes=44 * 2**20
        ),
    )(
        *(
            pltpu.with_memory_space_constraint(value, pltpu.HBM)
            for value in (
                prompt,
                norm_gain.reshape(1, width),
                gate.reshape(tp_n, flat, width),
                up.reshape(tp_n, flat, width),
                down.reshape(tp_n, flat, width),
                group_pick.reshape(1, tokens),
                route_weight.T,
            )
        )
    )
    gate_serve, up_serve, down_serve, mixed = pl.pallas_call(
        finish_kernel,
        out_shape=(served, served, served, jax.ShapeDtypeStruct((tokens, model), bf16)),
        in_specs=[anywhere, anywhere, anywhere, vmem, vmem],
        out_specs=(hbm,) * 4,
        scratch_shapes=[pltpu.VMEM((tokens, model), bf16), dma((3,)), dma((tp_n // 2,))],
        compiler_params=pltpu.CompilerParams(vmem_limit_bytes=16 * 2**20),
    )(gate_v, up_v, down_v, ret.reshape(tp_n // 2, block, 2 * width), placing)
    shape = (1, experts, units, model)
    return gate_serve.reshape(shape), up_serve.reshape(shape), down_serve.reshape(shape), mixed


def per_device(prompt, norm_gain, gate_master, up_master, down_master, group_pick, route_weight):
    group_total = lax.axis_size("tp")
    fs_n = lax.axis_size("fs")
    tok_count = prompt.shape[0]
    capacity = 2 * tok_count // group_total
    slot_total = group_total * capacity
    width, units = gate_master.shape[3], gate_master.shape[2]
    small = group_total == 8 and fs_n == 4
    if small and width % (2 * LANES) == 0 and units % LANES == 0 and capacity % 16 == 0:
        return fused_device(
            fs_n, gate_master, up_master, down_master,
            prompt, norm_gain, group_pick, route_weight, capacity,
        )
    gate_local = (gate_master * norm_gain).astype(jnp.bfloat16)
    up_local = (up_master * norm_gain).astype(jnp.bfloat16)
    down_local = down_master.astype(jnp.bfloat16)
    values = prompt.astype(jnp.float32)
    normed = (values * lax.rsqrt(jnp.mean(values * values, axis=1, keepdims=True) + EPS)).astype(
        jnp.bfloat16
    )
    chosen = group_pick[:, 0]
    member = (chosen[:, None] == jnp.arange(group_total, dtype=jnp.int32)[None, :]).astype(
        jnp.int32
    )
    slot_rank = jnp.sum(jnp.cumsum(member, axis=0) * member, axis=1) - 1
    target = chosen * capacity + slot_rank
    placing = (jnp.arange(slot_total, dtype=jnp.int32)[:, None] == target[None, :]).astype(
        jnp.bfloat16
    )
    gate_serve, up_serve, down_serve = (
        lax.all_to_all(gate_local, "tp", split_axis=0, concat_axis=3, tiled=True),
        lax.all_to_all(up_local, "tp", split_axis=0, concat_axis=3, tiled=True),
        lax.all_to_all(down_local, "tp", split_axis=0, concat_axis=3, tiled=True),
    )
    send_rows = jnp.dot(placing, normed, preferred_element_type=jnp.float32).astype(jnp.bfloat16)
    send_weights = jnp.dot(placing, route_weight, preferred_element_type=jnp.float32).astype(
        jnp.bfloat16
    )
    got_rows, got_weights = (
        lax.all_to_all(
            send_rows.reshape(group_total, capacity, -1),
            "tp",
            split_axis=0,
            concat_axis=0,
            tiled=True,
        ),
        lax.all_to_all(
            send_weights.reshape(group_total, capacity, -1),
            "tp",
            split_axis=0,
            concat_axis=0,
            tiled=True,
        ),
    )
    group_rows = got_rows.reshape(slot_total, -1)
    weights = got_weights.reshape(slot_total, -1)
    gathered = (
        lax.all_gather(gate_serve, "fs", axis=2, tiled=True),
        lax.all_gather(up_serve, "fs", axis=2, tiled=True),
        lax.all_gather(down_serve, "fs", axis=2, tiled=True),
    )
    summed = expert_rows(group_rows, weights, gathered)
    result = summed.astype(jnp.bfloat16).reshape(group_total, capacity, -1)
    returned = lax.all_to_all(result, "tp", split_axis=0, concat_axis=0, tiled=True)
    mixed = jnp.einsum(
        "st,sd->td", placing, returned.reshape(slot_total, -1), preferred_element_type=jnp.float32
    ).astype(jnp.bfloat16)
    return (gate_serve, up_serve, down_serve, mixed)


def solution(mesh):
    placed = (
        P(("fs", "tp"), None),
        P("tp"),
        P(None, None, "fs", "tp"),
        P(None, None, "fs", "tp"),
        P(None, None, "fs", "tp"),
        P(("fs", "tp"), None),
        P(("fs", "tp"), None),
    )
    return jax.shard_map(
        per_device,
        mesh=mesh,
        in_specs=placed,
        out_specs=(
            P("tp", None, "fs", None),
            P("tp", None, "fs", None),
            P("tp", None, "fs", None),
            P(("fs", "tp"), None),
        ),
        check_vma=False,
    )
```
